128 devices in a mesh: fs: 16 (over z, x), tp: 8 (over y, core).
Axes of the slice: x: 4, y: 4, z: 4, core: 2. Of those that a mesh axis runs over, the one named last changes fastest.
Arguments:
- normed_input: bfloat16 [32768, 2048], P('fs'), may hold values from -6 to 6
- output_cotangent: bfloat16 [32768, 2048], P('fs'), may hold values from -6 to 6
- query_grad: bfloat16 [32768, 2048], P('fs', 'tp'), may hold values from -0.53033009 to 0.53033009
- key_grad: bfloat16 [32768, 2048], P('fs', 'tp'), may hold values from -0.53033009 to 0.53033009
- attn_values: bfloat16 [32768, 2048], P('fs', 'tp'), may hold values from -0.53033009 to 0.53033009
- master_weights: float32 [3, 2048, 2048], P(None, 'fs', 'tp'), may hold values from -3 to 3
- factors: bfloat16 [3, 2048, 256], P(None, 'fs'), may hold values from -0.375 to 0.375
- moments: float32 [3, 256, 2048], P(None, 'fs', 'tp'), may hold values from -620 to 620
Outputs:
- new_weights: float32 [3, 2048, 2048], P(None, 'fs', 'tp')
- weight_copies: bfloat16 [3, 2048, 2048], P(None, None, 'tp')
- steps: float32 [3, 2048, 2048], P(None, 'fs', 'tp')
- new_moments: float32 [3, 256, 2048], P(None, 'fs', 'tp')
The draws below stay inside these ranges and needn't reach their ends.
All inputs are finite; a program needn't handle non-finite values.
Results may differ from the reference program's by a relative error of at most 0.0055.
Values may be sent and summed in bfloat16 or wider, within the bound.
No kernel may reach another device: no remote copies, remote signals or barrier semaphores. Data moves between devices by JAX's collectives and lax.ppermute only.
A program may use at most 128 MiB of HBM per device.

```python
import jax
import jax.numpy as jnp
from jax import lax

D = 2048
RANK = 256
TOKENS = 32768


def column_law(key, rows, cols):
    first, second = jax.random.split(key)
    column = jnp.arange(cols, dtype=jnp.float32)
    rough = jax.random.uniform(second, (cols,), jnp.float32, 0.6, 1.6)
    scale = 10.0 ** (column / max(cols - 1, 1)) * rough
    base = jnp.clip(jax.random.normal(first, (rows, cols), jnp.float32), -6.0, 6.0)
    return base * scale[None, :]


def draw_query_grad(key, part):
    return (column_law(jax.random.fold_in(key, 11), TOKENS, D) * TOKENS ** (-0.5)).astype(jnp.bfloat16)


def draw_key_grad(key, part):
    return (column_law(jax.random.fold_in(key, 12), TOKENS, D) * TOKENS ** (-0.5)).astype(jnp.bfloat16)


def draw_attn_values(key, part):
    return (column_law(jax.random.fold_in(key, 13), TOKENS, D) * TOKENS ** (-0.5)).astype(jnp.bfloat16)


def draw_moments(key, part):
    blocks = []
    for index in range(3):
        inner = jax.random.fold_in(key, 20 + index)
        values = column_law(inner, RANK, D)
        row = jnp.arange(RANK, dtype=jnp.float32)
        lift = 10.0 ** (0.5 * row / max(RANK - 1, 1))
        blocks.append(2.0 * values * lift[:, None])
    return jnp.stack(blocks).astype(jnp.float32)


def block_levels(rng, dims, cuts, low, top_value):
    def one(axis_at, shards_of):
        steps = jax.random.uniform(jax.random.fold_in(jax.random.fold_in(rng, 6), axis_at), (shards_of,), jnp.float32, low / len(cuts), top_value / len(cuts))
        return jnp.repeat(jnp.exp(steps), dims[axis_at] // shards_of).reshape((-1,) + (1,) * (len(dims) - axis_at - 1))

    loudness = one(*cuts[0])
    for cut in cuts[1:]:
        loudness = loudness * one(*cut)
    return loudness


def centred(stream_key, dims, width, reach, cuts=(), kind=jnp.bfloat16):
    result = jax.random.normal(stream_key, dims, jnp.float32) * width
    if len(cuts) > 0:
        result = block_levels(stream_key, dims, cuts, -0.22, 0.18) * result
    return jnp.clip(result, min=-reach, max=reach).astype(kind)


def setup_inputs(seed: int = 0) -> dict:
    arg_keys = jax.random.split(jax.random.key(seed), 9)
    return {
        "normed_input": centred(arg_keys[0], (TOKENS, D), 1.0, 6.0, ((0, 16),)),
        "output_cotangent": centred(arg_keys[1], (TOKENS, D), 1.0, 6.0, ((0, 16),)),
        "query_grad": draw_query_grad(jax.random.fold_in(arg_keys[8], 71), 0),
        "key_grad": draw_key_grad(jax.random.fold_in(arg_keys[8], 71), 0),
        "attn_values": draw_attn_values(jax.random.fold_in(arg_keys[8], 71), 0),
        "master_weights": centred(arg_keys[5], (3, D, D), 0.5, 3.0, ((1, 16), (2, 8)), jnp.float32),
        "factors": centred(arg_keys[6], (3, D, RANK), RANK ** -0.5, 0.375, ((1, 16),)),
        "moments": draw_moments(jax.random.fold_in(arg_keys[8], 71), 0),
    }


def reference(normed_input, output_cotangent, query_grad, key_grad, attn_values, master_weights, factors, moments):
    pairs = ((normed_input, query_grad), (normed_input, key_grad), (output_cotangent, attn_values))
    updated = []
    for index in range(3):
        left, right = pairs[index]
        gradient = jnp.dot(left.T, right, preferred_element_type=jnp.float32)
        projected = jnp.dot(factors[index].astype(jnp.float32).T, gradient, precision=lax.Precision.HIGHEST)
        updated.append(0.8 * moments[index] + 0.2 * projected)
    new_moments = jnp.stack(updated)
    rms = jnp.sqrt(jnp.mean(new_moments * new_moments) + 1e-06)
    normalized = (new_moments / rms).astype(jnp.bfloat16)
    steps = jnp.stack([jnp.dot(factors[index], normalized[index], preferred_element_type=jnp.float32) for index in range(3)])
    new_weights = master_weights - 0.05 * steps
    return (new_weights, new_weights.astype(jnp.bfloat16), steps, new_moments)
```

```python
import jax
import jax.numpy as jnp
from jax import lax
from jax.experimental import pallas as pl
from jax.experimental.pallas import tpu as pltpu
from jax.sharding import Mesh
from jax.sharding import PartitionSpec as P

Z, X, Y, C = "fs_0", "fs_1", "tp_0", "tp_1"
FS = (Z, X)
TP = (Y, C)
BF = jnp.bfloat16
F32 = jnp.float32


def shift(value, axis, by):
    n = lax.axis_size(axis)
    return lax.ppermute(value, axis, [(i, (i + by) % n) for i in range(n)])


def round_axis(value, axis):
    return [value] + [shift(value, axis, k) for k in (1, 2, 3)]


def swap(value):
    return lax.ppermute(value, C, [(0, 1), (1, 0)])


def vmem(count):
    return [pl.BlockSpec(memory_space=pltpu.VMEM) for _ in range(count)]


def call(kernel, outs, args, scratch=()):
    return pl.pallas_call(
        kernel,
        out_shape=outs,
        in_specs=vmem(len(args)),
        out_specs=vmem(len(outs)),
        scratch_shapes=list(scratch),
        compiler_params=pltpu.CompilerParams(vmem_limit_bytes=56 * 1024 * 1024),
    )(*args)


def behind(index, by):
    return lax.rem(index - by + 4, 4)


def gather_factors(factors):
    core = lax.axis_index(C)
    half = lax.dynamic_slice_in_dim(factors, core * 64, 64, axis=1)
    a, b = half[:, :32], half[:, 32:]
    first = jnp.stack(round_axis(a, X))
    second = jnp.stack(round_axis(b, Z))
    mine = round_axis(first, Z) + round_axis(second, X)
    return mine + [swap(m) for m in mine]


def project_kernel(*refs):
    blocks, grads = refs[:16], refs[16:19]
    whole = refs[19]
    a_out, b_out = refs[20:24], refs[24:28]
    total = refs[28]
    z, x, core = lax.axis_index(Z), lax.axis_index(X), lax.axis_index(C)
    for half in range(2):
        lane = core if half == 0 else 1 - core
        for which in range(2):
            for far in range(4):
                block = blocks[half * 8 + which * 4 + far]
                for near in range(4):
                    if which == 0:
                        owner = behind(z, far) * 4 + behind(x, near)
                    else:
                        owner = behind(z, near) * 4 + behind(x, far)
                    row = pl.multiple_of(owner * 128 + lane * 64 + which * 32, 32)
                    for j in range(3):
                        whole[j, pl.ds(row, 32), :] = block[near, j]
    for j in range(3):
        total[j] = lax.dot_general(whole[j], grads[j][...], (((0,), (0,)), ((), ())), preferred_element_type=F32)
    for k in range(4):
        xa, za = lax.rem(x + k, 4), lax.rem(z + k, 4)
        for j in range(3):
            for s in range(4):
                row = pl.multiple_of(64 * s + 16 * xa, 16)
                a_out[k][j, s] = total[j, pl.ds(row, 16), 0:128].astype(a_out[k].dtype)
                row = pl.multiple_of(64 * za + 16 * s, 16)
                b_out[k][j, s] = total[j, pl.ds(row, 16), 128:256].astype(b_out[k].dtype)


def moment_kernel(*refs):
    a_sums, b_sums, a_mom, b_mom, own = refs[0:4], refs[4:8], refs[8:12], refs[12:16], refs[16]
    a_new, b_new, own_new = refs[17:20]
    a_slots, b_slots = refs[20:22]
    z, x = lax.axis_index(Z), lax.axis_index(X)
    for k in range(4):
        a_slots[behind(z, k)] = a_sums[k][...]
        b_slots[behind(x, k)] = b_sums[k][...]
    for k in range(4):
        za, xa = behind(z, k), behind(x, k)
        for j in range(3):
            s = (a_slots[0, j, za].astype(F32) + a_slots[1, j, za].astype(F32)) + (
                a_slots[2, j, za].astype(F32) + a_slots[3, j, za].astype(F32)
            )
            m = 0.8 * a_mom[k][j] + 0.2 * s
            a_new[j, za] = m.astype(BF)
            if k == 0:
                own_new[j, :, 0:128] = m
            s = (b_slots[0, j, xa].astype(F32) + b_slots[1, j, xa].astype(F32)) + (
                b_slots[2, j, xa].astype(F32) + b_slots[3, j, xa].astype(F32)
            )
            m = 0.8 * b_mom[k][j] + 0.2 * s
            b_new[j, xa] = m.astype(BF)
            if k == 0:
                own_new[j, :, 128:256] = m


def join_kernel(*refs):
    a_parts, b_parts = refs[0:4], refs[4:8]
    joined, squares = refs[8:10]
    z, x = lax.axis_index(Z), lax.axis_index(X)
    for k in range(4):
        za, xa = behind(z, k), behind(x, k)
        for j in range(3):
            for s in range(4):
                joined[j, pl.ds(pl.multiple_of(64 * s + 16 * xa, 16), 16), 0:128] = a_parts[k][j, s]
                joined[j, pl.ds(pl.multiple_of(64 * za + 16 * s, 16), 16), 128:256] = b_parts[k][j, s]
    acc = jnp.zeros((8, 256), F32)
    for j in range(3):
        m = joined[j].astype(F32)
        acc = acc + jnp.sum((m * m).reshape(32, 8, 256), axis=0)
    squares[...] = jnp.broadcast_to(jnp.sum(acc, axis=(0, 1), keepdims=True), (8, 128))


def update_kernel(entries, *refs):
    parts = refs[0:4]
    joined, whole, factors, master = refs[4:8]
    blocks = refs[8:16]
    new_weights, copies, steps = refs[16:19]
    z, x, y = lax.axis_index(Z), lax.axis_index(X), lax.axis_index(Y)
    values = [p[0:1, 0:1] for p in parts]
    ordered = []
    for a in range(4):
        k = behind(y, a)
        v = jnp.where(k == 0, values[0], jnp.where(k == 1, values[1], jnp.where(k == 2, values[2], values[3])))
        ordered.append(v)
    total = (ordered[0] + ordered[1]) + (ordered[2] + ordered[3])
    inverse = lax.rsqrt(total / entries + 1e-06)
    scale = 0.05 * inverse
    for j in range(3):
        own = jnp.dot(factors[j], joined[j], preferred_element_type=F32) * inverse
        steps[j] = own
        new_weights[j] = master[j] - 0.05 * own
    for which in range(2):
        for far in range(4):
            block = blocks[which * 4 + far]
            for near in range(4):
                if which == 0:
                    owner = behind(z, far) * 4 + behind(x, near)
                else:
                    owner = behind(z, near) * 4 + behind(x, far)
                row = pl.ds(pl.multiple_of(owner * 128 + which * 64, 64), 64)
                for j in range(3):
                    back = jnp.dot(whole[j, row, :], joined[j], preferred_element_type=F32)
                    copies[j, row, :] = (block[near, j].astype(F32) - scale * back).astype(BF)


def on_device(
    normed_input,
    output_cotangent,
    query_grad,
    key_grad,
    attn_values,
    master_weights,
    factors,
    moments,
):
    pieces = gather_factors(factors)
    contract = (((0,), (0,)), ((), ()))
    grads = [
        lax.dot_general(left, right, contract, preferred_element_type=F32).astype(BF)
        for left, right in ((normed_input, query_grad), (normed_input, key_grad), (output_cotangent, attn_values))
    ]
    a_mom = round_axis(moments[:, :, 0:128], Z)
    b_mom = round_axis(moments[:, :, 128:256], X)
    rounded = master_weights.astype(BF)
    first = jnp.stack(round_axis(rounded[:, :64], X))
    second = jnp.stack(round_axis(rounded[:, 64:], Z))
    weight_blocks = round_axis(first, Z) + round_axis(second, X)

    part = (3, 4, 16, 128)
    part_types = [jax.ShapeDtypeStruct(part, F32)] + [jax.ShapeDtypeStruct(part, BF)] * 3
    out = call(
        project_kernel,
        [jax.ShapeDtypeStruct((3, 2048, 256), BF)] + part_types + part_types,
        pieces + grads,
        [pltpu.VMEM((3, 256, 256), F32)],
    )
    whole = out[0]
    a_sum, b_sum = out[1], out[5]
    for k in (1, 2, 3):
        a_sum = a_sum + shift(out[1 + k], X, k).astype(F32)
        b_sum = b_sum + shift(out[5 + k], Z, k).astype(F32)
    a_sums = round_axis(a_sum.astype(BF), Z)
    b_sums = round_axis(b_sum.astype(BF), X)
    bf_part = jax.ShapeDtypeStruct(part, BF)
    a_new, b_new, new_moments = call(
        moment_kernel,
        [bf_part, bf_part, jax.ShapeDtypeStruct((3, 16, 256), F32)],
        a_sums + b_sums + a_mom + b_mom + [moments],
        [pltpu.VMEM((4, *part), BF), pltpu.VMEM((4, *part), BF)],
    )
    joined, squares = call(
        join_kernel,
        [jax.ShapeDtypeStruct((3, 256, 256), BF), jax.ShapeDtypeStruct((8, 128), F32)],
        round_axis(a_new, X) + round_axis(b_new, Z),
    )
    pair = squares + swap(squares)
    shards = round_axis(pair, Y)
    entries = 3 * 256 * 2048
    new_weights, weight_copies, steps = call(
        lambda *refs: update_kernel(entries, *refs),
        [
            jax.ShapeDtypeStruct((3, 128, 256), F32),
            jax.ShapeDtypeStruct((3, 2048, 256), BF),
            jax.ShapeDtypeStruct((3, 128, 256), F32),
        ],
        shards + [joined, whole, factors, master_weights] + weight_blocks,
    )
    return (new_weights, weight_copies, steps, new_moments)


def solution(mesh):
    split = Mesh(mesh.devices.reshape(4, 4, 4, 2), (Z, X, Y, C))
    placed = (
        P(FS, None),
        P(FS, None),
        P(FS, TP),
        P(FS, TP),
        P(FS, TP),
        P(None, FS, TP),
        P(None, FS, None),
        P(None, FS, TP),
    )
    return jax.shard_map(
        on_device,
        mesh=split,
        in_specs=placed,
        out_specs=(P(None, FS, TP), P(None, None, TP), P(None, FS, TP), P(None, FS, TP)),
        check_vma=False,
    )
```

```python
import jax
import jax.numpy as jnp
from jax import lax
from jax.experimental import pallas as pl
from jax.experimental.pallas import tpu as pltpu
from jax.sharding import Mesh
from jax.sharding import PartitionSpec as P


Z, X, Y, C = "fs_0", "fs_1", "tp_0", "tp_1"
FS = (Z, X)
TP = (Y, C)
BF = jnp.bfloat16
F32 = jnp.float32


def swap(value):
    return lax.ppermute(value, C, [(0, 1), (1, 0)])


def turn(value, first, by):
    pairs = []
    for z in range(4):
        for x in range(4):
            for y in range(4):
                for c in range(2):
                    along_x = (c == 0) == first
                    to_z, to_x = (z, (x + by) % 4) if along_x else ((z + by) % 4, x)
                    pairs.append((((z * 4 + x) * 4 + y) * 2 + c, ((to_z * 4 + to_x) * 4 + y) * 2 + c))
    return lax.ppermute(value, FS + TP, pairs)


def exchange(value, axes):
    return lax.all_to_all(value, axes, 0, 0, tiled=True)


def vmem(count):
    return [pl.BlockSpec(memory_space=pltpu.VMEM) for _ in range(count)]


def hbm(count):
    return [pl.BlockSpec(memory_space=pltpu.HBM) for _ in range(count)]


def call(kernel, outs, args, scratch=(), mib=16, ins=None, out_specs=None):
    return pl.pallas_call(
        kernel,
        out_shape=outs,
        in_specs=ins or vmem(len(args)),
        out_specs=out_specs or vmem(len(outs)),
        scratch_shapes=list(scratch),
        compiler_params=pltpu.CompilerParams(vmem_limit_bytes=mib * 1024 * 1024),
    )(*args)


def behind(index, by):
    return lax.rem(index - by + 4, 4)


def after(value, *others):
    return lax.optimization_barrier((value, *others))[0]


def spread_kernel(factors, out):
    row = pl.multiple_of(lax.axis_index(C) * 64, 64)
    half = factors[:, pl.ds(row, 64), :]
    for f in range(16):
        out[f] = half


def gradient_kernel(first, second, q, k, v, out, a, b, sides, turned, acc, a_sems, b_sems, side_sems):
    halves = [pl.ds(0, 1024), pl.ds(1024, 1024)]
    side_loads = [pltpu.make_async_copy(r, sides.at[j], side_sems.at[j]) for j, r in enumerate((q, k, v))]
    a_loads = [pltpu.make_async_copy(first.at[h], a.at[h], a_sems.at[i]) for i, h in enumerate(halves)]
    b_loads = [pltpu.make_async_copy(second.at[h], b.at[h], b_sems.at[i]) for i, h in enumerate(halves)]
    for load in side_loads[:2] + a_loads[:1] + side_loads[2:] + a_loads[1:] + b_loads:
        load.start()
    for j in range(2):
        side_loads[j].wait()
        turned[256 * j : 256 * j + 256, :] = sides[j].T
    a_loads[0].wait()

    @pl.loop(0, 8)
    def _(i):
        cols = pl.ds(pl.multiple_of(i * 256, 256), 256)
        acc[:, cols] = jnp.dot(turned[0:512, 0:1024], a[0:1024, cols], preferred_element_type=F32)

    side_loads[2].wait()
    turned[512:768, :] = sides[2].T
    a_loads[1].wait()

    @pl.loop(0, 8)
    def _(i):
        cols = pl.ds(pl.multiple_of(i * 256, 256), 256)
        found = acc[:, cols] + jnp.dot(turned[0:512, 1024:2048], a[1024:2048, cols], preferred_element_type=F32)
        out[0, :, cols] = found[0:256].astype(BF)
        out[1, :, cols] = found[256:512].astype(BF)

    for load in b_loads:
        load.wait()

    @pl.loop(0, 8)
    def _(i):
        cols = pl.ds(pl.multiple_of(i * 256, 256), 256)
        out[2, :, cols] = jnp.dot(turned[512:768, :], b[:, cols], preferred_element_type=F32).astype(BF)


def gradients(*args):
    (out,) = call(
        gradient_kernel,
        [jax.ShapeDtypeStruct((3, 256, 2048), BF)],
        args,
        [
            pltpu.VMEM((2048, 2048), BF),
            pltpu.VMEM((2048, 2048), BF),
            pltpu.VMEM((3, 2048, 256), BF),
            pltpu.VMEM((768, 2048), BF),
            pltpu.VMEM((512, 2048), F32),
            pltpu.SemaphoreType.DMA((2,)),
            pltpu.SemaphoreType.DMA((2,)),
            pltpu.SemaphoreType.DMA((3,)),
        ],
        mib=58,
        ins=hbm(5),
    )
    return out


def project_kernel(mine, mate, grads, parts, whole):
    core = lax.axis_index(C)
    here = pl.multiple_of(core * 64, 64)
    there = pl.multiple_of((1 - core) * 64, 64)
    for f in range(16):
        for j in range(3):
            whole[j, pl.ds(f * 128 + here, 64), :] = mine[f, j]
            whole[j, pl.ds(f * 128 + there, 64), :] = mate[f, j]
    for j in range(3):
        total = jnp.dot(grads[j], whole[j], preferred_element_type=F32).T
        for f in range(16):
            parts[f, j] = total[16 * f : 16 * f + 16, :].astype(BF)


def moment_kernel(parts, moments, spread, new_moments):
    for j in range(3):
        s = parts[0, j].astype(F32)
        for f in range(1, 16):
            s = s + parts[f, j].astype(F32)
        m = 0.8 * moments[j] + 0.2 * s
        new_moments[j] = m
        rounded = m.astype(BF)
        for f in range(16):
            spread[f, j] = rounded


def join_kernel(gathered, joined, squares):
    acc = jnp.zeros((16, 256), F32)
    for j in range(3):
        for f in range(16):
            block = gathered[f, j]
            joined[j, 16 * f : 16 * f + 16, :] = block
            wide = block.astype(F32)
            acc = acc + wide * wide
    squares[...] = jnp.broadcast_to(jnp.sum(acc, axis=(0, 1), keepdims=True).reshape(1, 1, 1), squares.shape)


def back_kernel(joined, factors, mine, mate, found, own, whole, made, own_sems, mate_sems, out_sems):
    core = lax.axis_index(C)
    here = pl.multiple_of(core * 64, 64)
    there = pl.multiple_of((1 - core) * 64, 64)
    pairs = []
    for f in range(16):
        pairs.append(
            (
                pltpu.make_async_copy(mine.at[f], whole.at[:, pl.ds(f * 128 + here, 64), :], own_sems.at[f]),
                pltpu.make_async_copy(mate.at[f], whole.at[:, pl.ds(f * 128 + there, 64), :], mate_sems.at[f]),
            )
        )
    for a, b in pairs:
        a.start()
        b.start()
    for j in range(3):
        own[j] = jnp.dot(factors[j], joined[j], preferred_element_type=F32)
    stores = []
    for chunk in range(4):
        for a, b in pairs[4 * chunk : 4 * chunk + 4]:
            a.wait()
            b.wait()
        rows = pl.ds(512 * chunk, 512)
        for j in range(3):
            made[j, rows, :] = jnp.dot(whole[j, rows, :], joined[j], preferred_element_type=F32).astype(BF)
        store = pltpu.make_async_copy(made.at[:, rows, :], found.at[:, rows, :], out_sems.at[chunk])
        store.start()
        stores.append(store)
    for store in stores:
        store.wait()


def update_kernel(entries, squares, found, own, master, line, back, low, high, front, *refs):
    new_weights, steps, copies = refs[0:3]
    blocks, backs, made, block_sems, back_sems, out_sems = refs[3:9]
    z, x, core = lax.axis_index(Z), lax.axis_index(X), lax.axis_index(C)
    loads = []
    count = 0
    for far, source, nears in (
        (0, line, (0, 1, 2, 3)),
        (1, back, (0, 1, 2, 3)),
        (2, low, (0, 1)),
        (2, high, (2, 3)),
        (3, front, (0, 1, 2, 3)),
    ):
        for near in nears:
            owner = jnp.where(
                core == 0,
                behind(z, far) * 4 + behind(x, near),
                behind(z, near) * 4 + behind(x, far),
            )
            row = pl.multiple_of(owner * 128, 128)
            loads.append(
                pltpu.make_async_copy(
                    source.at[near - nears[0]], blocks.at[:, pl.ds(row, 128), :], block_sems.at[count]
                )
            )
            count += 1
    for load in loads:
        load.start()
    fills = []
    for chunk in range(4):
        rows = pl.ds(512 * chunk, 512)
        fill = pltpu.make_async_copy(found.at[:, rows, :], backs.at[:, rows, :], back_sems.at[chunk])
        fill.start()
        fills.append(fill)
    sums = jnp.sum(squares[...], axis=(0, 1))
    inverse = lax.rsqrt(sums.reshape(1, 128)[0:1, 0:1] / entries + 1e-06)
    scale = 0.05 * inverse
    for j in range(3):
        step = own[j] * inverse
        steps[j] = step
        new_weights[j] = master[j] - 0.05 * step
    for load in loads:
        load.wait()
    stores = []
    for chunk in range(4):
        rows = pl.ds(512 * chunk, 512)
        fills[chunk].wait()
        for j in range(3):
            made[j, rows, :] = (blocks[j, rows, :].astype(F32) - scale * backs[j, rows, :].astype(F32)).astype(BF)
        store = pltpu.make_async_copy(made.at[:, rows, :], copies.at[:, rows, :], out_sems.at[chunk])
        store.start()
        stores.append(store)
    for store in stores:
        store.wait()


def on_device(
    normed_input,
    output_cotangent,
    query_grad,
    key_grad,
    attn_values,
    master_weights,
    factors,
    moments,
):
    (spread,) = call(spread_kernel, [jax.ShapeDtypeStruct((16, 3, 64, 256), BF)], [factors])
    mine = exchange(spread, FS)

    own = master_weights.astype(BF)
    near_back = turn(own, True, 1)
    near_front = turn(own, True, -1)
    grads = gradients(normed_input, output_cotangent, query_grad, key_grad, attn_values)
    mine = after(mine, grads)
    mate = swap(mine)
    near_low = turn(after(near_back, mine)[:, :64], True, 1)
    near_high = turn(after(near_front, mine)[:, 64:], True, -1)
    line = jnp.stack([own, near_back, jnp.concatenate([near_low, near_high], axis=1), near_front])

    back = turn(line, False, 1)
    front = turn(line, False, -1)

    (parts,) = call(
        project_kernel,
        [jax.ShapeDtypeStruct((16, 3, 16, 256), BF)],
        [mine, mate, grads],
        [pltpu.VMEM((3, 2048, 256), BF)],
    )
    received = exchange(parts, FS)
    normal, new_moments = call(
        moment_kernel,
        [jax.ShapeDtypeStruct((16, 3, 16, 256), BF), jax.ShapeDtypeStruct((3, 16, 256), F32)],
        [received, moments],
    )
    gathered = exchange(normal, FS)
    joined, squares = call(
        join_kernel,
        [jax.ShapeDtypeStruct((3, 256, 256), BF), jax.ShapeDtypeStruct((8, 1, 128), F32)],
        [gathered],
    )
    all_squares = exchange(squares, TP)
    low = turn(back[:2], False, 1)
    high = turn(front[2:], False, -1)

    entries = 3 * 256 * 2048
    shard = jax.ShapeDtypeStruct((3, 128, 256), F32)
    found, own_found = call(
        back_kernel,
        [jax.ShapeDtypeStruct((3, 2048, 256), BF), shard],
        [joined, factors, mine, mate],
        [
            pltpu.VMEM((3, 2048, 256), BF),
            pltpu.VMEM((3, 2048, 256), BF),
            pltpu.SemaphoreType.DMA((16,)),
            pltpu.SemaphoreType.DMA((16,)),
            pltpu.SemaphoreType.DMA((4,)),
        ],
        mib=58,
        ins=vmem(2) + hbm(2),
        out_specs=hbm(1) + vmem(1),
    )
    new_weights, steps, weight_copies = call(
        lambda *refs: update_kernel(entries, *refs),
        [shard, shard, jax.ShapeDtypeStruct((3, 2048, 256), BF)],
        [all_squares, found, own_found, master_weights, line, back, low, high, front],
        [
            pltpu.VMEM((3, 2048, 256), BF),
            pltpu.VMEM((3, 2048, 256), BF),
            pltpu.VMEM((3, 2048, 256), BF),
            pltpu.SemaphoreType.DMA((16,)),
            pltpu.SemaphoreType.DMA((4,)),
            pltpu.SemaphoreType.DMA((4,)),
        ],
        mib=58,
        ins=vmem(1) + hbm(1) + vmem(2) + hbm(5),
        out_specs=vmem(2) + hbm(1),
    )
    return (new_weights, weight_copies, steps, new_moments)


def solution(mesh):
    split = Mesh(mesh.devices.reshape(4, 4, 4, 2), (Z, X, Y, C))
    placed = (
        P(FS, None),
        P(FS, None),
        P(FS, TP),
        P(FS, TP),
        P(FS, TP),
        P(None, FS, TP),
        P(None, FS, None),
        P(None, FS, TP),
    )

    return jax.shard_map(
        on_device,
        mesh=split,
        in_specs=placed,
        out_specs=(P(None, FS, TP), P(None, None, TP), P(None, FS, TP), P(None, FS, TP)),
        check_vma=False,
    )
```

```python
import jax
import jax.numpy as jnp
from jax import lax
from jax.experimental import pallas as pl
from jax.experimental.pallas import tpu as pltpu
from jax.sharding import Mesh
from jax.sharding import PartitionSpec as P


Z, X, Y, C = "fs_0", "fs_1", "tp_0", "tp_1"
FS = (Z, X)
TP = (Y, C)
BF = jnp.bfloat16
F32 = jnp.float32


def swap(value):
    return lax.ppermute(value, C, [(0, 1), (1, 0)])


def turn(value, first, by):
    pairs = []
    for z in range(4):
        for x in range(4):
            for y in range(4):
                for c in range(2):
                    along_x = (c == 0) == first
                    to_z, to_x = (z, (x + by) % 4) if along_x else ((z + by) % 4, x)
                    pairs.append((((z * 4 + x) * 4 + y) * 2 + c, ((to_z * 4 + to_x) * 4 + y) * 2 + c))
    return lax.ppermute(value, FS + TP, pairs)


def exchange(value, axes):
    return lax.all_to_all(value, axes, 0, 0, tiled=True)


def vmem(count):
    return [pl.BlockSpec(memory_space=pltpu.VMEM) for _ in range(count)]


def hbm(count):
    return [pl.BlockSpec(memory_space=pltpu.HBM) for _ in range(count)]


def call(kernel, outs, args, scratch=(), mib=16, ins=None, out_specs=None):
    return pl.pallas_call(
        kernel,
        out_shape=outs,
        in_specs=ins or vmem(len(args)),
        out_specs=out_specs or vmem(len(outs)),
        scratch_shapes=list(scratch),
        compiler_params=pltpu.CompilerParams(vmem_limit_bytes=mib * 1024 * 1024),
    )(*args)


def behind(index, by):
    return lax.rem(index - by + 4, 4)


def after(value, *others):
    return lax.optimization_barrier((value, *others))[0]


def spread_kernel(factors, out, half, sem, sems):
    row = pl.multiple_of(lax.axis_index(C) * 64, 64)
    load = pltpu.make_async_copy(factors.at[:, pl.ds(row, 64), :], half, sem)
    load.start()
    load.wait()
    moves = [pltpu.make_async_copy(half, out.at[f], sems.at[f]) for f in range(16)]
    for move in moves:
        move.start()
    for move in moves:
        move.wait()


def gradient_kernel(first, second, q, k, v, out, a, b, sides, left_sems, side_sems):
    for source, target, sem in (
        (q, sides.at[0], side_sems.at[0]),
        (k, sides.at[1], side_sems.at[1]),
        (first, a, left_sems.at[0]),
        (v, sides.at[2], side_sems.at[2]),
        (second, b, left_sems.at[1]),
    ):
        for i in range(8):
            rows = pl.ds(256 * i, 256)
            pltpu.make_async_copy(source.at[rows], target.at[rows], sem).start()
    for j, (side, left, block) in enumerate(((q, first, a), (k, first, a), (v, second, b))):
        pltpu.make_async_copy(side, sides.at[j], side_sems.at[j]).wait()
        if j != 1:
            pltpu.make_async_copy(left, block, left_sems.at[j // 2]).wait()
        out[j] = lax.dot_general(
            sides[j], block[...], (((0,), (0,)), ((), ())), preferred_element_type=F32
        ).astype(BF)


def held_in_hbm(values):
    return [pltpu.with_memory_space_constraint(v, pltpu.HBM) for v in values]


def gradients(*args):
    (out,) = call(
        gradient_kernel,
        [jax.ShapeDtypeStruct((3, 256, 2048), BF)],
        held_in_hbm(args),
        [
            pltpu.VMEM((2048, 2048), BF),
            pltpu.VMEM((2048, 2048), BF),
            pltpu.VMEM((3, 2048, 256), BF),
            pltpu.SemaphoreType.DMA((2,)),
            pltpu.SemaphoreType.DMA((3,)),
        ],
        mib=32,
        ins=hbm(5),
    )
    return out


def project_kernel(mine, mate, grads, parts, whole):
    core = lax.axis_index(C)
    here = pl.multiple_of(core * 64, 64)
    there = pl.multiple_of((1 - core) * 64, 64)
    for j in range(3):
        for f in range(16):
            whole[j, pl.ds(f * 128 + here, 64), :] = mine[f, j]
            whole[j, pl.ds(f * 128 + there, 64), :] = mate[f, j]
        total = jnp.dot(grads[j], whole[j], preferred_element_type=F32).T
        for f in range(16):
            parts[f, j] = total[16 * f : 16 * f + 16, :].astype(BF)


def moment_kernel(parts, held, spread, new_moments):
    for j in range(3):
        s = parts[0, j].astype(F32)
        for f in range(1, 16):
            s = s + parts[f, j].astype(F32)
        m = held[j] + 0.2 * s
        new_moments[j] = m
        rounded = m.astype(BF)
        for f in range(16):
            spread[f, j] = rounded


def join_kernel(gathered, squares):
    acc = jnp.zeros((16, 256), F32)
    for j in range(3):
        for f in range(16):
            wide = gathered[f, j].astype(F32)
            acc = acc + wide * wide
    squares[...] = jnp.broadcast_to(jnp.sum(acc, axis=(0, 1), keepdims=True).reshape(1, 1, 1), squares.shape)


def stack_kernel(own, back_top, back_bottom, low, high, front_top, front_bottom, moments, near, far, held):
    near[0] = own[...]
    near[1, :, 0:64, :] = back_top[...]
    near[1, :, 64:128, :] = back_bottom[...]
    far[0, :, 0:64, :] = low[...]
    far[0, :, 64:128, :] = high[...]
    far[1, :, 0:64, :] = front_top[...]
    far[1, :, 64:128, :] = front_bottom[...]
    held[...] = 0.8 * moments[...]


def update_kernel(entries, squares, gathered, far_first, far_last, factors, master, mine, mate, *refs):
    sources = refs[0:6]
    new_weights, steps, copies = refs[6:9]
    factors_v, master_v, weights_v, steps_v, joined, whole, blocks, made = refs[9:17]
    small_sems, whole_sems, block_sems, out_sems = refs[17:21]
    z, x, core = lax.axis_index(Z), lax.axis_index(X), lax.axis_index(C)
    small = [
        pltpu.make_async_copy(source, target, small_sems.at[i])
        for i, (source, target) in enumerate(
            ((factors, factors_v), (master, master_v))
        )
    ]
    owners, kept = [], []
    for far in range(4):
        for near in range(4):
            owner = jnp.where(
                core == 0,
                behind(z, far) * 4 + behind(x, near),
                behind(z, near) * 4 + behind(x, far),
            )
            row = pl.multiple_of(owner * 128, 128)
            if far == 2:
                kept.append(((far_first, far_last)[near // 2], near % 2, row))
            else:
                owners.append((sources[(0, 2, 0, 4)[far] + near // 2], near % 2, row))
    here = pl.multiple_of(core * 64, 64)
    there = pl.multiple_of((1 - core) * 64, 64)
    for j in range(3):
        for f in range(16):
            pltpu.make_async_copy(
                mine.at[f, j], whole.at[j, pl.ds(f * 128 + here, 64), :], whole_sems.at[j]
            ).start()
            pltpu.make_async_copy(
                mate.at[f, j], whole.at[j, pl.ds(f * 128 + there, 64), :], whole_sems.at[j]
            ).start()
        for source, slot, row in owners:
            pltpu.make_async_copy(source.at[slot, j], blocks.at[j, pl.ds(row, 128), :], block_sems.at[j]).start()
        if j == 0:
            for load in small:
                load.start()
    for source, slot, row in kept:
        for j in range(3):
            blocks[j, pl.ds(row, 128), :] = source[slot, j]
    sums = jnp.sum(squares[...], axis=(0, 1))
    inverse = lax.rsqrt(sums.reshape(1, 128)[0:1, 0:1] / entries + 1e-06)
    scale = 0.05 * inverse
    for j in range(3):
        for f in range(16):
            joined[j, 16 * f : 16 * f + 16, :] = gathered[f, j]
    small[0].wait()
    small[1].wait()
    stores = []
    for j in range(3):
        step = jnp.dot(factors_v[j], joined[j], preferred_element_type=F32) * inverse
        steps_v[j] = step
        weights_v[j] = master_v[j] - 0.05 * step
    stores.append(pltpu.make_async_copy(steps_v, steps, out_sems.at[6]))
    stores.append(pltpu.make_async_copy(weights_v, new_weights, out_sems.at[7]))
    for store in stores:
        store.start()
    for j in range(3):
        pltpu.make_async_copy(copies.at[j], whole.at[j], whole_sems.at[j]).wait()
        pltpu.make_async_copy(copies.at[j, 0:1536], blocks.at[j, 0:1536], block_sems.at[j]).wait()
        for half in range(2):
            for part in range(2):
                rows = pl.ds(1024 * half + 512 * part, 512)
                found = jnp.dot(whole[j, rows, :], joined[j], preferred_element_type=F32)
                made[j, rows, :] = (blocks[j, rows, :].astype(F32) - scale * found).astype(BF)
            rows = pl.ds(1024 * half, 1024)
            store = pltpu.make_async_copy(made.at[j, rows, :], copies.at[j, rows, :], out_sems.at[2 * j + half])
            store.start()
            stores.append(store)
    for store in stores:
        store.wait()


def on_device(
    normed_input,
    output_cotangent,
    query_grad,
    key_grad,
    attn_values,
    master_weights,
    factors,
    moments,
):
    (spread,) = call(
        spread_kernel,
        [jax.ShapeDtypeStruct((16, 3, 64, 256), BF)],
        [factors],
        [pltpu.VMEM((3, 64, 256), BF), pltpu.SemaphoreType.DMA, pltpu.SemaphoreType.DMA((16,))],
        mib=58,
        ins=hbm(1),
        out_specs=hbm(1),
    )
    mine = exchange(spread, FS)

    own = master_weights.astype(BF)
    top, bottom = own[:, :64], own[:, 64:]
    back_top = turn(top, True, 1)
    back_bottom = turn(bottom, True, 1)
    front_top = turn(top, True, -1)
    front_bottom = turn(bottom, True, -1)

    grads = gradients(normed_input, output_cotangent, query_grad, key_grad, attn_values)
    mine = after(mine, grads)
    mate = swap(mine)
    low = turn(after(back_top, mine), True, 1)
    high = turn(after(front_bottom, mine), True, -1)
    (parts,) = call(
        project_kernel,
        [jax.ShapeDtypeStruct((16, 3, 16, 256), BF)],
        [mine, mate, grads],
        [pltpu.VMEM((3, 2048, 256), BF)],
    )
    received = exchange(parts, FS)
    pair = jax.ShapeDtypeStruct((2, 3, 128, 256), BF)
    first, last, held = call(
        stack_kernel,
        [pair, pair, jax.ShapeDtypeStruct((3, 16, 256), F32)],
        [after(own, parts), back_top, back_bottom, low, high, front_top, front_bottom, moments],
    )
    back_first = turn(first, False, 1)
    back_last = turn(last, False, 1)
    front_first = turn(first, False, -1)
    front_last = turn(last, False, -1)
    normal, new_moments = call(
        moment_kernel,
        [jax.ShapeDtypeStruct((16, 3, 16, 256), BF), jax.ShapeDtypeStruct((3, 16, 256), F32)],
        [received, held],
    )
    gathered = exchange(normal, FS)
    far_first = turn(after(back_first, normal), False, 1)
    far_last = turn(after(front_last, normal), False, -1)
    (squares,) = call(join_kernel, [jax.ShapeDtypeStruct((8, 1, 128), F32)], [gathered])
    all_squares = exchange(squares, TP)
    entries = 3 * 256 * 2048
    shard = jax.ShapeDtypeStruct((3, 128, 256), F32)
    fixed = [factors, master_weights, mine, mate, first, last, back_first, back_last, front_first, front_last]
    args = [all_squares, gathered, far_first, far_last] + held_in_hbm(fixed)
    new_weights, steps, weight_copies = call(
        lambda *refs: update_kernel(entries, *refs),
        [shard, shard, jax.ShapeDtypeStruct((3, 2048, 256), BF)],
        args,
        [
            pltpu.VMEM((3, 128, 256), BF),
            pltpu.VMEM((3, 128, 256), F32),
            pltpu.VMEM((3, 128, 256), F32),
            pltpu.VMEM((3, 128, 256), F32),
            pltpu.VMEM((3, 256, 256), BF),
            pltpu.VMEM((3, 2048, 256), BF),
            pltpu.VMEM((3, 2048, 256), BF),
            pltpu.VMEM((3, 2048, 256), BF),
            pltpu.SemaphoreType.DMA((2,)),
            pltpu.SemaphoreType.DMA((3,)),
            pltpu.SemaphoreType.DMA((3,)),
            pltpu.SemaphoreType.DMA((8,)),
        ],
        mib=20,
        ins=vmem(4) + hbm(10),
        out_specs=hbm(3),
    )
    return (new_weights, weight_copies, steps, new_moments)


def solution(mesh):
    split = Mesh(mesh.devices.reshape(4, 4, 4, 2), (Z, X, Y, C))
    placed = (
        P(FS, None),
        P(FS, None),
        P(FS, TP),
        P(FS, TP),
        P(FS, TP),
        P(None, FS, TP),
        P(None, FS, None),
        P(None, FS, TP),
    )

    return jax.shard_map(
        on_device,
        mesh=split,
        in_specs=placed,
        out_specs=(P(None, FS, TP), P(None, None, TP), P(None, FS, TP), P(None, FS, TP)),
        check_vma=False,
    )
```

```python
import jax
import jax.numpy as jnp
from jax import lax
from jax.experimental import pallas as pl
from jax.experimental.pallas import tpu as pltpu
from jax.sharding import Mesh
from jax.sharding import PartitionSpec as P


Z, X, Y, C = "fs_0", "fs_1", "tp_0", "tp_1"
FS = (Z, X)
TP = (Y, C)
BF = jnp.bfloat16
F32 = jnp.float32


def swap(value):
    return lax.ppermute(value, C, [(0, 1), (1, 0)])


def turn(value, first, by):
    pairs = []
    for z in range(4):
        for x in range(4):
            for y in range(4):
                for c in range(2):
                    along_x = (c == 0) == first
                    to_z, to_x = (z, (x + by) % 4) if along_x else ((z + by) % 4, x)
                    pairs.append((((z * 4 + x) * 4 + y) * 2 + c, ((to_z * 4 + to_x) * 4 + y) * 2 + c))
    return lax.ppermute(value, FS + TP, pairs)


def exchange(value, axes):
    return lax.all_to_all(value, axes, 0, 0, tiled=True)


def vmem(count):
    return [pl.BlockSpec(memory_space=pltpu.VMEM) for _ in range(count)]


def hbm(count):
    return [pl.BlockSpec(memory_space=pltpu.HBM) for _ in range(count)]


def call(kernel, outs, args, scratch=(), mib=16, ins=None, out_specs=None):
    return pl.pallas_call(
        kernel,
        out_shape=outs,
        in_specs=ins or vmem(len(args)),
        out_specs=out_specs or vmem(len(outs)),
        scratch_shapes=list(scratch),
        compiler_params=pltpu.CompilerParams(vmem_limit_bytes=mib * 1024 * 1024),
    )(*args)


def behind(index, by):
    return lax.rem(index - by + 4, 4)


def after(value, *others):
    return lax.optimization_barrier((value, *others))[0]


def spread_kernel(factors, out, half, sem, sems):
    lanes = pl.ds(pl.multiple_of(lax.axis_index(C) * 128, 128), 128)
    load = pltpu.make_async_copy(factors.at[:, :, lanes], half, sem)
    load.start()
    load.wait()
    moves = [pltpu.make_async_copy(half, out.at[f], sems.at[f]) for f in range(16)]
    for move in moves:
        move.start()
    for move in moves:
        move.wait()


def gradient_kernel(first, second, q, k, v, out, a, b, sides, made, left_sems, side_sems, out_sems):
    def loads(source, target, sem, cols):
        for i in range(4):
            rows = pl.ds(512 * i, 512)
            pltpu.make_async_copy(source.at[rows, cols], target.at[rows, cols], sem).start()

    def wait(source, target, sem, cols):
        pltpu.make_async_copy(source.at[:, cols], target.at[:, cols], sem).wait()

    full = pl.ds(0, 256)
    halves = (pl.ds(0, 1024), pl.ds(1024, 1024))
    loads(q, sides.at[0], side_sems.at[0], full)
    loads(first, a, left_sems.at[0], halves[0])
    loads(k, sides.at[1], side_sems.at[1], full)
    loads(first, a, left_sems.at[1], halves[1])
    loads(v, sides.at[2], side_sems.at[2], full)
    loads(second, b, left_sems.at[2], halves[0])
    loads(second, b, left_sems.at[3], halves[1])
    stores = []
    done = set()
    for step, (j, half) in enumerate(((0, 0), (1, 0), (0, 1), (1, 1), (2, 0), (2, 1))):
        side, left, block = ((q, first, a), (k, first, a), (v, second, b))[j]
        if j not in done:
            done.add(j)
            wait(side, sides.at[j], side_sems.at[j], full)
        part = 2 * (j // 2) + half
        if j != 1:
            wait(left, block, left_sems.at[part], halves[half])
        made[j, :, halves[half]] = lax.dot_general(
            sides[j], block[:, halves[half]], (((0,), (0,)), ((), ())), preferred_element_type=F32
        ).astype(BF)
        store = pltpu.make_async_copy(made.at[j, :, halves[half]], out.at[j, :, halves[half]], out_sems.at[step])
        store.start()
        stores.append(store)
    for store in stores:
        store.wait()


def held_in_hbm(values):
    return [pltpu.with_memory_space_constraint(v, pltpu.HBM) for v in values]


def gradients(*args):
    (out,) = call(
        gradient_kernel,
        [jax.ShapeDtypeStruct((3, 256, 2048), BF)],
        args,
        [
            pltpu.VMEM((2048, 2048), BF),
            pltpu.VMEM((2048, 2048), BF),
            pltpu.VMEM((3, 2048, 256), BF),
            pltpu.VMEM((3, 256, 2048), BF),
            pltpu.SemaphoreType.DMA((4,)),
            pltpu.SemaphoreType.DMA((3,)),
            pltpu.SemaphoreType.DMA((6,)),
        ],
        mib=58,
        ins=hbm(5),
        out_specs=hbm(1),
    )
    return out


def side_kernel(mine, grads, kept, part, sems):
    loads = [pltpu.make_async_copy(grads.at[j], kept.at[j], sems.at[j]) for j in range(3)]
    for load in loads:
        load.start()
    for j in range(3):
        loads[j].wait()
        whole = mine[:, j].reshape(2048, 128)
        part[j] = jnp.dot(kept[j], whole, preferred_element_type=F32).T.astype(BF)


def project_kernel(mate, grads, part, parts):
    core = lax.axis_index(C)
    here, there = core * 8, 8 - core * 8
    for j in range(3):
        whole = mate[:, j].reshape(2048, 128)
        other = jnp.dot(grads[j], whole, preferred_element_type=F32).T.astype(BF)
        for i in range(8):
            parts[here + i, j] = part[j, 16 * i : 16 * i + 16, :]
            parts[there + i, j] = other[16 * i : 16 * i + 16, :]


def moment_kernel(parts, held, spread, new_moments):
    for j in range(3):
        s = parts[0, j].astype(F32)
        for f in range(1, 16):
            s = s + parts[f, j].astype(F32)
        m = held[j] + 0.2 * s
        new_moments[j] = m
        rounded = m.astype(BF)
        for f in range(16):
            spread[f, j] = rounded


def join_kernel(gathered, squares):
    acc = jnp.zeros((16, 256), F32)
    for j in range(3):
        for f in range(16):
            wide = gathered[f, j].astype(F32)
            acc = acc + wide * wide
    squares[...] = jnp.broadcast_to(jnp.sum(acc, axis=(0, 1), keepdims=True).reshape(1, 1, 1), squares.shape)


def stack_kernel(own, back_top, back_bottom, low, high, front_top, front_bottom, moments, line, held, raw, sem):
    load = pltpu.make_async_copy(moments, raw, sem)
    load.start()
    line[0] = own[...]
    line[1, :, 0:64, :] = back_top[...]
    line[1, :, 64:128, :] = back_bottom[...]
    line[2, :, 0:64, :] = low[...]
    line[2, :, 64:128, :] = high[...]
    line[3, :, 0:64, :] = front_top[...]
    line[3, :, 64:128, :] = front_bottom[...]
    load.wait()
    held[...] = 0.8 * raw[...]


def update_kernel(entries, squares, gathered, far_first, far_last, factors, master, mine, mate, *refs):
    line, back, front = refs[0:3]
    new_weights, steps, copies = refs[3:6]
    factors_v, master_v, weights_v, steps_v, joined, whole, blocks, made = refs[6:14]
    small_sems, whole_sems, block_sems, out_sems = refs[14:18]
    z, x, core = lax.axis_index(Z), lax.axis_index(X), lax.axis_index(C)
    small = [
        pltpu.make_async_copy(source, target, small_sems.at[i])
        for i, (source, target) in enumerate(
            ((factors, factors_v), (master, master_v))
        )
    ]
    owners, kept = [], []
    for far in range(4):
        for near in range(4):
            owner = jnp.where(
                core == 0,
                behind(z, far) * 4 + behind(x, near),
                behind(z, near) * 4 + behind(x, far),
            )
            row = pl.multiple_of(owner * 128, 128)
            if far == 2:
                kept.append(((far_first, far_last)[near // 2], near % 2, row))
            else:
                owners.append(((line, back, None, front)[far], near, row))
    here = pl.ds(pl.multiple_of(core * 128, 128), 128)
    there = pl.ds(pl.multiple_of(128 - core * 128, 128), 128)
    whole_loads = []
    for j in range(3):
        for side, (source, lanes) in enumerate(((mine, here), (mate, there))):
            whole_loads.append(
                pltpu.make_async_copy(source.at[:, j], whole.at[j, :, :, lanes], whole_sems.at[j, side])
            )
    block_loads = []
    for i, (source, slot, row) in enumerate(owners):
        block_loads.append(pltpu.make_async_copy(source.at[slot], blocks.at[:, pl.ds(row, 128), :], block_sems.at[i]))
    for load in small + whole_loads[:2] + block_loads + whole_loads[2:]:
        load.start()
    for source, slot, row in kept:
        for j in range(3):
            blocks[j, pl.ds(row, 128), :] = source[slot, j]
    sums = jnp.sum(squares[...], axis=(0, 1))
    inverse = lax.rsqrt(sums.reshape(1, 128)[0:1, 0:1] / entries + 1e-06)
    scale = 0.05 * inverse
    for j in range(3):
        for f in range(16):
            joined[j, 16 * f : 16 * f + 16, :] = gathered[f, j]
    small[0].wait()
    small[1].wait()
    stores = []
    for j in range(3):
        step = jnp.dot(factors_v[j], joined[j], preferred_element_type=F32) * inverse
        steps_v[j] = step
        weights_v[j] = master_v[j] - 0.05 * step
    stores.append(pltpu.make_async_copy(steps_v, steps, out_sems.at[12]))
    stores.append(pltpu.make_async_copy(weights_v, new_weights, out_sems.at[13]))
    for store in stores:
        store.start()
    for load in block_loads:
        load.wait()
    for j in range(3):
        for load in whole_loads[2 * j : 2 * j + 2]:
            load.wait()
        for part in range(4):
            rows = pl.ds(512 * part, 512)
            side = whole[j, 4 * part : 4 * part + 4].reshape(512, 256)
            found = jnp.dot(side, joined[j], preferred_element_type=F32)
            made[j, rows, :] = (blocks[j, rows, :].astype(F32) - scale * found).astype(BF)
            if part % 2 == 1 or j == 2:
                rows = pl.ds(512 * part, 512) if j == 2 else pl.ds(512 * part - 512, 1024)
                store = pltpu.make_async_copy(made.at[j, rows, :], copies.at[j, rows, :], out_sems.at[4 * j + part])
                store.start()
                stores.append(store)
    for store in stores:
        store.wait()


def on_device(
    normed_input,
    output_cotangent,
    query_grad,
    key_grad,
    attn_values,
    master_weights,
    factors,
    moments,
):
    (spread,) = call(
        spread_kernel,
        [jax.ShapeDtypeStruct((16, 3, 128, 128), BF)],
        [factors],
        [pltpu.VMEM((3, 128, 128), BF), pltpu.SemaphoreType.DMA, pltpu.SemaphoreType.DMA((16,))],
        mib=58,
        ins=hbm(1),
        out_specs=hbm(1),
    )
    mine = exchange(spread, FS)

    own = master_weights.astype(BF)
    top, bottom = own[:, :64], own[:, 64:]
    back_top = turn(top, True, 1)
    back_bottom = turn(bottom, True, 1)
    front_top = turn(top, True, -1)
    front_bottom = turn(bottom, True, -1)

    grads = gradients(normed_input, output_cotangent, query_grad, key_grad, attn_values)
    mine = after(mine, grads)
    mate = swap(mine)
    low = turn(after(back_top, mine), True, 1)
    high = turn(after(front_bottom, mine), True, -1)
    kept, part = call(
        side_kernel,
        [jax.ShapeDtypeStruct((3, 256, 2048), BF), jax.ShapeDtypeStruct((3, 128, 256), BF)],
        [mine] + held_in_hbm([grads]),
        [pltpu.SemaphoreType.DMA((3,))],
        ins=vmem(1) + hbm(1),
    )
    (parts,) = call(
        project_kernel,
        [jax.ShapeDtypeStruct((16, 3, 16, 256), BF)],
        [mate, kept, part],
    )
    received = exchange(parts, FS)
    line, held = call(
        stack_kernel,
        [jax.ShapeDtypeStruct((4, 3, 128, 256), BF), jax.ShapeDtypeStruct((3, 16, 256), F32)],
        [after(own, parts), back_top, back_bottom, low, high, front_top, front_bottom] + held_in_hbm([moments]),
        [pltpu.VMEM((3, 16, 256), F32), pltpu.SemaphoreType.DMA],
        ins=vmem(7) + hbm(1),
    )
    back = turn(line, False, 1)
    front = turn(line, False, -1)
    normal, new_moments = call(
        moment_kernel,
        [jax.ShapeDtypeStruct((16, 3, 16, 256), BF), jax.ShapeDtypeStruct((3, 16, 256), F32)],
        [received, held],
    )
    gathered = exchange(normal, FS)
    far_first = turn(after(back, normal)[:2], False, 1)
    far_last = turn(after(front, normal)[2:], False, -1)
    (squares,) = call(join_kernel, [jax.ShapeDtypeStruct((8, 1, 128), F32)], [gathered])
    all_squares = exchange(squares, TP)
    entries = 3 * 256 * 2048
    shard = jax.ShapeDtypeStruct((3, 128, 256), F32)
    fixed = [factors, master_weights, mine, mate, line, back, front]
    args = [all_squares, gathered, far_first, far_last] + held_in_hbm(fixed)
    new_weights, steps, weight_copies = call(
        lambda *refs: update_kernel(entries, *refs),
        [shard, shard, jax.ShapeDtypeStruct((3, 2048, 256), BF)],
        args,
        [
            pltpu.VMEM((3, 128, 256), BF),
            pltpu.VMEM((3, 128, 256), F32),
            pltpu.VMEM((3, 128, 256), F32),
            pltpu.VMEM((3, 128, 256), F32),
            pltpu.VMEM((3, 256, 256), BF),
            pltpu.VMEM((3, 16, 128, 256), BF),
            pltpu.VMEM((3, 2048, 256), BF),
            pltpu.VMEM((3, 2048, 256), BF),
            pltpu.SemaphoreType.DMA((2,)),
            pltpu.SemaphoreType.DMA((3, 2)),
            pltpu.SemaphoreType.DMA((12,)),
            pltpu.SemaphoreType.DMA((14,)),
        ],
        mib=20,
        ins=vmem(4) + hbm(7),
        out_specs=hbm(3),
    )
    return (new_weights, weight_copies, steps, new_moments)


def solution(mesh):
    split = Mesh(mesh.devices.reshape(4, 4, 4, 2), (Z, X, Y, C))
    placed = (
        P(FS, None),
        P(FS, None),
        P(FS, TP),
        P(FS, TP),
        P(FS, TP),
        P(None, FS, TP),
        P(None, FS, None),
        P(None, FS, TP),
    )

    return jax.shard_map(
        on_device,
        mesh=split,
        in_specs=placed,
        out_specs=(P(None, FS, TP), P(None, None, TP), P(None, FS, TP), P(None, FS, TP)),
        check_vma=False,
    )
```

```python
import jax
import jax.numpy as jnp
from jax import lax
from jax.experimental import pallas as pl
from jax.experimental.pallas import tpu as pltpu
from jax.sharding import Mesh
from jax.sharding import PartitionSpec as P


Z, X, Y, C = "fs_0", "fs_1", "tp_0", "tp_1"
FS = (Z, X)
TP = (Y, C)
BF = jnp.bfloat16
F32 = jnp.float32


def swap(value):
    return lax.ppermute(value, C, [(0, 1), (1, 0)])


def turn(value, first, by):
    pairs = []
    for z in range(4):
        for x in range(4):
            for y in range(4):
                for c in range(2):
                    along_x = (c == 0) == first
                    to_z, to_x = (z, (x + by) % 4) if along_x else ((z + by) % 4, x)
                    pairs.append((((z * 4 + x) * 4 + y) * 2 + c, ((to_z * 4 + to_x) * 4 + y) * 2 + c))
    return lax.ppermute(value, FS + TP, pairs)


def exchange(value, axes):
    return lax.all_to_all(value, axes, 0, 0, tiled=True)


def vmem(count):
    return [pl.BlockSpec(memory_space=pltpu.VMEM) for _ in range(count)]


def hbm(count):
    return [pl.BlockSpec(memory_space=pltpu.HBM) for _ in range(count)]


def call(kernel, outs, args, scratch=(), mib=16, ins=None, out_specs=None):
    return pl.pallas_call(
        kernel,
        out_shape=outs,
        in_specs=ins or vmem(len(args)),
        out_specs=out_specs or vmem(len(outs)),
        scratch_shapes=list(scratch),
        compiler_params=pltpu.CompilerParams(vmem_limit_bytes=mib * 1024 * 1024),
    )(*args)


def behind(index, by):
    return lax.rem(index - by + 4, 4)


def after(value, *others):
    return lax.optimization_barrier((value, *others))[0]


def spread_kernel(factors, out, half, sem, sems):
    lanes = pl.ds(pl.multiple_of(lax.axis_index(C) * 128, 128), 128)
    load = pltpu.make_async_copy(factors.at[:, :, lanes], half, sem)
    load.start()
    load.wait()
    moves = [pltpu.make_async_copy(half, out.at[f], sems.at[f]) for f in range(16)]
    for move in moves:
        move.start()
    for move in moves:
        move.wait()


def gradient_kernel(first, second, q, k, v, out, a, b, sides, made, left_sems, side_sems, out_sems):
    def loads(source, target, sem, cols):
        for i in range(4):
            rows = pl.ds(512 * i, 512)
            pltpu.make_async_copy(source.at[rows, cols], target.at[rows, cols], sem).start()

    def wait(source, target, sem, cols):
        pltpu.make_async_copy(source.at[:, cols], target.at[:, cols], sem).wait()

    full = pl.ds(0, 256)
    halves = (pl.ds(0, 1024), pl.ds(1024, 1024))
    loads(q, sides.at[0], side_sems.at[0], full)
    loads(first, a, left_sems.at[0], halves[0])
    loads(k, sides.at[1], side_sems.at[1], full)
    loads(first, a, left_sems.at[1], halves[1])
    loads(v, sides.at[2], side_sems.at[2], full)
    loads(second, b, left_sems.at[2], halves[0])
    loads(second, b, left_sems.at[3], halves[1])
    stores = []
    done = set()
    for step, (j, half) in enumerate(((0, 0), (1, 0), (0, 1), (1, 1), (2, 0), (2, 1))):
        side, left, block = ((q, first, a), (k, first, a), (v, second, b))[j]
        if j not in done:
            done.add(j)
            wait(side, sides.at[j], side_sems.at[j], full)
        part = 2 * (j // 2) + half
        if j != 1:
            wait(left, block, left_sems.at[part], halves[half])
        made[j, :, halves[half]] = lax.dot_general(
            sides[j], block[:, halves[half]], (((0,), (0,)), ((), ())), preferred_element_type=F32
        ).astype(BF)
        store = pltpu.make_async_copy(made.at[j, :, halves[half]], out.at[j, :, halves[half]], out_sems.at[step])
        store.start()
        stores.append(store)
    for store in stores:
        store.wait()


def held_in_hbm(values):
    return [pltpu.with_memory_space_constraint(v, pltpu.HBM) for v in values]


def gradients(*args):
    (out,) = call(
        gradient_kernel,
        [jax.ShapeDtypeStruct((3, 256, 2048), BF)],
        args,
        [
            pltpu.VMEM((2048, 2048), BF),
            pltpu.VMEM((2048, 2048), BF),
            pltpu.VMEM((3, 2048, 256), BF),
            pltpu.VMEM((3, 256, 2048), BF),
            pltpu.SemaphoreType.DMA((4,)),
            pltpu.SemaphoreType.DMA((3,)),
            pltpu.SemaphoreType.DMA((6,)),
        ],
        mib=58,
        ins=hbm(5),
        out_specs=hbm(1),
    )
    return out


def side_kernel(mine, grads, kept, part, sems):
    loads = [pltpu.make_async_copy(grads.at[j], kept.at[j], sems.at[j]) for j in range(3)]
    for load in loads:
        load.start()
    for j in range(3):
        loads[j].wait()
        whole = mine[:, j].reshape(2048, 128)
        part[j] = jnp.dot(kept[j], whole, preferred_element_type=F32).T.astype(BF)


def project_kernel(mate, grads, part, parts):
    core = lax.axis_index(C)
    here, there = core * 8, 8 - core * 8
    for j in range(3):
        whole = mate[:, j].reshape(2048, 128)
        other = jnp.dot(grads[j], whole, preferred_element_type=F32).T.astype(BF)
        for i in range(8):
            parts[here + i, j] = part[j, 16 * i : 16 * i + 16, :]
            parts[there + i, j] = other[16 * i : 16 * i + 16, :]


def moment_kernel(parts, held, spread, new_moments):
    for j in range(3):
        s = parts[0, j].astype(F32)
        for f in range(1, 16):
            s = s + parts[f, j].astype(F32)
        m = held[j] + 0.2 * s
        new_moments[j] = m
        rounded = m.astype(BF)
        for f in range(16):
            spread[f, j] = rounded


def join_kernel(gathered, squares):
    acc = jnp.zeros((16, 256), F32)
    for j in range(3):
        for f in range(16):
            wide = gathered[f, j].astype(F32)
            acc = acc + wide * wide
    squares[...] = jnp.broadcast_to(jnp.sum(acc, axis=(0, 1), keepdims=True).reshape(1, 1, 1), squares.shape)


def stack_kernel(own, near_back, opposite, near_front, moments, line, held, raw, sem):
    load = pltpu.make_async_copy(moments, raw, sem)
    load.start()
    for i, block in enumerate((own, near_back, opposite, near_front)):
        line[i] = block[...]
    load.wait()
    held[...] = 0.8 * raw[...]


def update_kernel(entries, squares, gathered, far_first, far_last, factors, master, mine, mate, *refs):
    line, back, front = refs[0:3]
    new_weights, steps, copies = refs[3:6]
    factors_v, master_v, weights_v, steps_v, joined, whole, blocks, made = refs[6:14]
    small_sems, whole_sems, block_sems, out_sems = refs[14:18]
    z, x, core = lax.axis_index(Z), lax.axis_index(X), lax.axis_index(C)
    small = [
        pltpu.make_async_copy(source, target, small_sems.at[i])
        for i, (source, target) in enumerate(
            ((factors, factors_v), (master, master_v))
        )
    ]
    owners, kept = [], []
    for far in range(4):
        for near in range(4):
            owner = jnp.where(
                core == 0,
                behind(z, far) * 4 + behind(x, near),
                behind(z, near) * 4 + behind(x, far),
            )
            row = pl.multiple_of(owner * 128, 128)
            if far == 2:
                kept.append(((far_first, far_last)[near // 2], near % 2, row))
            else:
                owners.append(((line, back, None, front)[far], near, row))
    here = pl.ds(pl.multiple_of(core * 128, 128), 128)
    there = pl.ds(pl.multiple_of(128 - core * 128, 128), 128)
    whole_loads = []
    for j in range(3):
        for side, (source, lanes) in enumerate(((mine, here), (mate, there))):
            whole_loads.append(
                pltpu.make_async_copy(source.at[:, j], whole.at[j, :, :, lanes], whole_sems.at[j, side])
            )
    block_loads = []
    for i, (source, slot, row) in enumerate(owners):
        block_loads.append(pltpu.make_async_copy(source.at[slot], blocks.at[:, pl.ds(row, 128), :], block_sems.at[i]))
    for load in small + whole_loads[:2] + block_loads + whole_loads[2:]:
        load.start()
    for source, slot, row in kept:
        for j in range(3):
            blocks[j, pl.ds(row, 128), :] = source[slot, j]
    sums = jnp.sum(squares[...], axis=(0, 1))
    inverse = lax.rsqrt(sums.reshape(1, 128)[0:1, 0:1] / entries + 1e-06)
    scale = 0.05 * inverse
    for j in range(3):
        for f in range(16):
            joined[j, 16 * f : 16 * f + 16, :] = gathered[f, j]
    small[0].wait()
    small[1].wait()
    stores = []
    for j in range(3):
        step = jnp.dot(factors_v[j], joined[j], preferred_element_type=F32) * inverse
        steps_v[j] = step
        weights_v[j] = master_v[j] - 0.05 * step
    stores.append(pltpu.make_async_copy(steps_v, steps, out_sems.at[12]))
    stores.append(pltpu.make_async_copy(weights_v, new_weights, out_sems.at[13]))
    for store in stores:
        store.start()
    for load in block_loads:
        load.wait()
    for j in range(3):
        for load in whole_loads[2 * j : 2 * j + 2]:
            load.wait()
        for part in range(4):
            rows = pl.ds(512 * part, 512)
            side = whole[j, 4 * part : 4 * part + 4].reshape(512, 256)
            found = jnp.dot(side, joined[j], preferred_element_type=F32)
            made[j, rows, :] = (blocks[j, rows, :].astype(F32) - scale * found).astype(BF)
            if part % 2 == 1 or j == 2:
                rows = pl.ds(512 * part, 512) if j == 2 else pl.ds(512 * part - 512, 1024)
                store = pltpu.make_async_copy(made.at[j, rows, :], copies.at[j, rows, :], out_sems.at[4 * j + part])
                store.start()
                stores.append(store)
    for store in stores:
        store.wait()


def on_device(
    normed_input,
    output_cotangent,
    query_grad,
    key_grad,
    attn_values,
    master_weights,
    factors,
    moments,
):
    (spread,) = call(
        spread_kernel,
        [jax.ShapeDtypeStruct((16, 3, 128, 128), BF)],
        [factors],
        [pltpu.VMEM((3, 128, 128), BF), pltpu.SemaphoreType.DMA, pltpu.SemaphoreType.DMA((16,))],
        mib=58,
        ins=hbm(1),
        out_specs=hbm(1),
    )
    mine = exchange(spread, FS)

    own = master_weights.astype(BF)
    near_back = turn(own, True, 1)
    near_front = turn(own, True, -1)
    opposite = turn(own, True, 2)

    grads = gradients(normed_input, output_cotangent, query_grad, key_grad, attn_values)
    mine = after(mine, grads)
    mate = swap(mine)
    kept, part = call(
        side_kernel,
        [jax.ShapeDtypeStruct((3, 256, 2048), BF), jax.ShapeDtypeStruct((3, 128, 256), BF)],
        [mine] + held_in_hbm([grads]),
        [pltpu.SemaphoreType.DMA((3,))],
        ins=vmem(1) + hbm(1),
    )
    (parts,) = call(
        project_kernel,
        [jax.ShapeDtypeStruct((16, 3, 16, 256), BF)],
        [mate, kept, part],
    )
    received = exchange(parts, FS)
    line, held = call(
        stack_kernel,
        [jax.ShapeDtypeStruct((4, 3, 128, 256), BF), jax.ShapeDtypeStruct((3, 16, 256), F32)],
        [after(own, parts), near_back, opposite, near_front] + held_in_hbm([moments]),
        [pltpu.VMEM((3, 16, 256), F32), pltpu.SemaphoreType.DMA],
        ins=vmem(4) + hbm(1),
    )
    back = turn(line, False, 1)
    front = turn(line, False, -1)
    normal, new_moments = call(
        moment_kernel,
        [jax.ShapeDtypeStruct((16, 3, 16, 256), BF), jax.ShapeDtypeStruct((3, 16, 256), F32)],
        [received, held],
    )
    gathered = exchange(normal, FS)
    far_first = turn(after(back, normal)[:2], False, 1)
    far_last = turn(after(front, normal)[2:], False, -1)
    (squares,) = call(join_kernel, [jax.ShapeDtypeStruct((8, 1, 128), F32)], [gathered])
    all_squares = exchange(squares, TP)
    entries = 3 * 256 * 2048
    shard = jax.ShapeDtypeStruct((3, 128, 256), F32)
    fixed = [factors, master_weights, mine, mate, line, back, front]
    args = [all_squares, gathered, far_first, far_last] + held_in_hbm(fixed)
    new_weights, steps, weight_copies = call(
        lambda *refs: update_kernel(entries, *refs),
        [shard, shard, jax.ShapeDtypeStruct((3, 2048, 256), BF)],
        args,
        [
            pltpu.VMEM((3, 128, 256), BF),
            pltpu.VMEM((3, 128, 256), F32),
            pltpu.VMEM((3, 128, 256), F32),
            pltpu.VMEM((3, 128, 256), F32),
            pltpu.VMEM((3, 256, 256), BF),
            pltpu.VMEM((3, 16, 128, 256), BF),
            pltpu.VMEM((3, 2048, 256), BF),
            pltpu.VMEM((3, 2048, 256), BF),
            pltpu.SemaphoreType.DMA((2,)),
            pltpu.SemaphoreType.DMA((3, 2)),
            pltpu.SemaphoreType.DMA((12,)),
            pltpu.SemaphoreType.DMA((14,)),
        ],
        mib=20,
        ins=vmem(4) + hbm(7),
        out_specs=hbm(3),
    )
    return (new_weights, weight_copies, steps, new_moments)


def solution(mesh):
    split = Mesh(mesh.devices.reshape(4, 4, 4, 2), (Z, X, Y, C))
    placed = (
        P(FS, None),
        P(FS, None),
        P(FS, TP),
        P(FS, TP),
        P(FS, TP),
        P(None, FS, TP),
        P(None, FS, None),
        P(None, FS, TP),
    )

    return jax.shard_map(
        on_device,
        mesh=split,
        in_specs=placed,
        out_specs=(P(None, FS, TP), P(None, None, TP), P(None, FS, TP), P(None, FS, TP)),
        check_vma=False,
    )
```

```python
import jax
import jax.numpy as jnp
from jax import lax
from jax.experimental import pallas as pl
from jax.experimental.pallas import tpu as pltpu
from jax.sharding import Mesh
from jax.sharding import PartitionSpec as P


Z, X, Y, C = "fs_0", "fs_1", "tp_0", "tp_1"
FS = (Z, X)
TP = (Y, C)
BF = jnp.bfloat16
F32 = jnp.float32


def swap(value):
    return lax.ppermute(value, C, [(0, 1), (1, 0)])


def turn(value, first, by):
    pairs = []
    for z in range(4):
        for x in range(4):
            for y in range(4):
                for c in range(2):
                    along_x = (c == 0) == first
                    to_z, to_x = (z, (x + by) % 4) if along_x else ((z + by) % 4, x)
                    pairs.append((((z * 4 + x) * 4 + y) * 2 + c, ((to_z * 4 + to_x) * 4 + y) * 2 + c))
    return lax.ppermute(value, FS + TP, pairs)


def exchange(value, axes):
    return lax.all_to_all(value, axes, 0, 0, tiled=True)


def vmem(count):
    return [pl.BlockSpec(memory_space=pltpu.VMEM) for _ in range(count)]


def hbm(count):
    return [pl.BlockSpec(memory_space=pltpu.HBM) for _ in range(count)]


def call(kernel, outs, args, scratch=(), mib=16, ins=None, out_specs=None):
    return pl.pallas_call(
        kernel,
        out_shape=outs,
        in_specs=ins or vmem(len(args)),
        out_specs=out_specs or vmem(len(outs)),
        scratch_shapes=list(scratch),
        compiler_params=pltpu.CompilerParams(vmem_limit_bytes=mib * 1024 * 1024),
    )(*args)


def behind(index, by):
    return lax.rem(index - by + 4, 4)


def after(value, *others):
    return lax.optimization_barrier((value, *others))[0]


def spread_kernel(factors, out, half, sem, sems):
    lanes = pl.ds(pl.multiple_of(lax.axis_index(C) * 128, 128), 128)
    load = pltpu.make_async_copy(factors.at[:, :, lanes], half, sem)
    load.start()
    load.wait()
    moves = [pltpu.make_async_copy(half, out.at[f], sems.at[f]) for f in range(16)]
    for move in moves:
        move.start()
    for move in moves:
        move.wait()


def gradient_kernel(first, second, q, k, v, out, a, b, sides, made, left_sems, side_sems, out_sems):
    def loads(source, target, sem, cols):
        for i in range(4):
            rows = pl.ds(512 * i, 512)
            pltpu.make_async_copy(source.at[rows, cols], target.at[rows, cols], sem).start()

    def wait(source, target, sem, cols):
        pltpu.make_async_copy(source.at[:, cols], target.at[:, cols], sem).wait()

    full = pl.ds(0, 256)
    halves = (pl.ds(0, 1024), pl.ds(1024, 1024))
    loads(q, sides.at[0], side_sems.at[0], full)
    loads(first, a, left_sems.at[0], halves[0])
    loads(k, sides.at[1], side_sems.at[1], full)
    loads(first, a, left_sems.at[1], halves[1])
    loads(v, sides.at[2], side_sems.at[2], full)
    loads(second, b, left_sems.at[2], halves[0])
    loads(second, b, left_sems.at[3], halves[1])
    stores = []
    done = set()
    for step, (j, half) in enumerate(((0, 0), (1, 0), (0, 1), (1, 1), (2, 0), (2, 1))):
        side, left, block = ((q, first, a), (k, first, a), (v, second, b))[j]
        if j not in done:
            done.add(j)
            wait(side, sides.at[j], side_sems.at[j], full)
        part = 2 * (j // 2) + half
        if j != 1:
            wait(left, block, left_sems.at[part], halves[half])
        made[j, :, halves[half]] = lax.dot_general(
            sides[j], block[:, halves[half]], (((0,), (0,)), ((), ())), preferred_element_type=F32
        ).astype(BF)
        store = pltpu.make_async_copy(made.at[j, :, halves[half]], out.at[j, :, halves[half]], out_sems.at[step])
        store.start()
        stores.append(store)
    for store in stores:
        store.wait()


def held_in_hbm(values):
    return [pltpu.with_memory_space_constraint(v, pltpu.HBM) for v in values]


def gradients(*args):
    (out,) = call(
        gradient_kernel,
        [jax.ShapeDtypeStruct((3, 256, 2048), BF)],
        args,
        [
            pltpu.VMEM((2048, 2048), BF),
            pltpu.VMEM((2048, 2048), BF),
            pltpu.VMEM((3, 2048, 256), BF),
            pltpu.VMEM((3, 256, 2048), BF),
            pltpu.SemaphoreType.DMA((4,)),
            pltpu.SemaphoreType.DMA((3,)),
            pltpu.SemaphoreType.DMA((6,)),
        ],
        mib=58,
        ins=hbm(5),
        out_specs=hbm(1),
    )
    return out


def side_kernel(mine, grads, kept, part, sems):
    loads = [pltpu.make_async_copy(grads.at[j], kept.at[j], sems.at[j]) for j in range(3)]
    for load in loads:
        load.start()
    for j in range(3):
        loads[j].wait()
        whole = mine[:, j].reshape(2048, 128)
        part[j] = jnp.dot(kept[j], whole, preferred_element_type=F32).T.astype(BF)


def project_kernel(mate, grads, part, parts):
    core = lax.axis_index(C)
    here, there = core * 8, 8 - core * 8
    for j in range(3):
        whole = mate[:, j].reshape(2048, 128)
        other = jnp.dot(grads[j], whole, preferred_element_type=F32).T.astype(BF)
        for i in range(8):
            parts[here + i, j] = part[j, 16 * i : 16 * i + 16, :]
            parts[there + i, j] = other[16 * i : 16 * i + 16, :]


def moment_kernel(parts, held, spread, new_moments):
    for j in range(3):
        s = parts[0, j].astype(F32)
        for f in range(1, 16):
            s = s + parts[f, j].astype(F32)
        m = held[j] + 0.2 * s
        new_moments[j] = m
        rounded = m.astype(BF)
        for f in range(16):
            spread[f, j] = rounded


def join_kernel(gathered, squares):
    acc = jnp.zeros((16, 256), F32)
    for j in range(3):
        for f in range(16):
            wide = gathered[f, j].astype(F32)
            acc = acc + wide * wide
    squares[...] = jnp.broadcast_to(jnp.sum(acc, axis=(0, 1), keepdims=True).reshape(1, 1, 1), squares.shape)


def hold_kernel(moments, held):
    held[...] = 0.8 * moments[...]


def stack_kernel(own, near_back, opposite, near_front, held, line, kept, raw, sem):
    load = pltpu.make_async_copy(held, raw, sem)
    load.start()
    for i, block in enumerate((own, near_back, opposite, near_front)):
        line[i] = block[...]
    load.wait()
    kept[...] = raw[...]


def update_kernel(entries, squares, gathered, far_first, far_last, factors, master, mine, mate, *refs):
    line, back, front = refs[0:3]
    new_weights, steps, copies = refs[3:6]
    factors_v, master_v, weights_v, steps_v, joined, whole, blocks, made = refs[6:14]
    small_sems, whole_sems, block_sems, out_sems = refs[14:18]
    z, x, core = lax.axis_index(Z), lax.axis_index(X), lax.axis_index(C)
    small = [
        pltpu.make_async_copy(source, target, small_sems.at[i])
        for i, (source, target) in enumerate(
            ((factors, factors_v), (master, master_v))
        )
    ]
    owners, kept = [], []
    for far in range(4):
        for near in range(4):
            owner = jnp.where(
                core == 0,
                behind(z, far) * 4 + behind(x, near),
                behind(z, near) * 4 + behind(x, far),
            )
            row = pl.multiple_of(owner * 128, 128)
            if far == 2:
                kept.append(((far_first, far_last)[near // 2], near % 2, row))
            else:
                owners.append(((line, back, None, front)[far], near, row))
    here = pl.ds(pl.multiple_of(core * 128, 128), 128)
    there = pl.ds(pl.multiple_of(128 - core * 128, 128), 128)
    whole_loads = []
    for j in range(3):
        for side, (source, lanes) in enumerate(((mine, here), (mate, there))):
            whole_loads.append(
                pltpu.make_async_copy(source.at[:, j], whole.at[j, :, :, lanes], whole_sems.at[j, side])
            )
    block_loads = []
    for i, (source, slot, row) in enumerate(owners):
        block_loads.append(pltpu.make_async_copy(source.at[slot], blocks.at[:, pl.ds(row, 128), :], block_sems.at[i]))
    for load in small + whole_loads[:2] + block_loads + whole_loads[2:]:
        load.start()
    for source, slot, row in kept:
        for j in range(3):
            blocks[j, pl.ds(row, 128), :] = source[slot, j]
    sums = jnp.sum(squares[...], axis=(0, 1))
    inverse = lax.rsqrt(sums.reshape(1, 128)[0:1, 0:1] / entries + 1e-06)
    scale = 0.05 * inverse
    for j in range(3):
        for f in range(16):
            joined[j, 16 * f : 16 * f + 16, :] = gathered[f, j]
    small[0].wait()
    small[1].wait()
    stores = []
    for j in range(3):
        step = jnp.dot(factors_v[j], joined[j], preferred_element_type=F32) * inverse
        steps_v[j] = step
        weights_v[j] = master_v[j] - 0.05 * step
    stores.append(pltpu.make_async_copy(steps_v, steps, out_sems.at[12]))
    stores.append(pltpu.make_async_copy(weights_v, new_weights, out_sems.at[13]))
    for store in stores:
        store.start()
    for load in block_loads:
        load.wait()
    for j in range(3):
        for load in whole_loads[2 * j : 2 * j + 2]:
            load.wait()
        for part in range(4):
            rows = pl.ds(512 * part, 512)
            side = whole[j, 4 * part : 4 * part + 4].reshape(512, 256)
            found = jnp.dot(side, joined[j], preferred_element_type=F32)
            made[j, rows, :] = (blocks[j, rows, :].astype(F32) - scale * found).astype(BF)
            if part % 2 == 1 or j == 2:
                rows = pl.ds(512 * part, 512) if j == 2 else pl.ds(512 * part - 512, 1024)
                store = pltpu.make_async_copy(made.at[j, rows, :], copies.at[j, rows, :], out_sems.at[4 * j + part])
                store.start()
                stores.append(store)
    for store in stores:
        store.wait()


def on_device(
    normed_input,
    output_cotangent,
    query_grad,
    key_grad,
    attn_values,
    master_weights,
    factors,
    moments,
):
    (spread,) = call(
        spread_kernel,
        [jax.ShapeDtypeStruct((16, 3, 128, 128), BF)],
        [factors],
        [pltpu.VMEM((3, 128, 128), BF), pltpu.SemaphoreType.DMA, pltpu.SemaphoreType.DMA((16,))],
        mib=58,
        ins=hbm(1),
        out_specs=hbm(1),
    )
    mine = exchange(spread, FS)

    own = master_weights.astype(BF)
    grads = gradients(normed_input, output_cotangent, query_grad, key_grad, attn_values)
    late = after(own, grads)
    near_back = turn(late, True, 1)
    near_front = turn(late, True, -1)
    opposite = turn(late, True, 2)
    (held,) = call(hold_kernel, [jax.ShapeDtypeStruct((3, 16, 256), F32)], [moments])
    mine = after(mine, grads)
    mate = swap(mine)
    kept, part = call(
        side_kernel,
        [jax.ShapeDtypeStruct((3, 256, 2048), BF), jax.ShapeDtypeStruct((3, 128, 256), BF)],
        [mine] + held_in_hbm([grads]),
        [pltpu.SemaphoreType.DMA((3,))],
        ins=vmem(1) + hbm(1),
    )
    (parts,) = call(
        project_kernel,
        [jax.ShapeDtypeStruct((16, 3, 16, 256), BF)],
        [mate, kept, part],
    )
    received = exchange(parts, FS)
    line, held = call(
        stack_kernel,
        [jax.ShapeDtypeStruct((4, 3, 128, 256), BF), jax.ShapeDtypeStruct((3, 16, 256), F32)],
        [after(own, parts), near_back, opposite, near_front] + held_in_hbm([held]),
        [pltpu.VMEM((3, 16, 256), F32), pltpu.SemaphoreType.DMA],
        ins=vmem(4) + hbm(1),
    )
    back = turn(line, False, 1)
    front = turn(line, False, -1)
    normal, new_moments = call(
        moment_kernel,
        [jax.ShapeDtypeStruct((16, 3, 16, 256), BF), jax.ShapeDtypeStruct((3, 16, 256), F32)],
        [received, held],
    )
    gathered = exchange(normal, FS)
    far_first = turn(after(back, normal)[:2], False, 1)
    far_last = turn(after(front, normal)[2:], False, -1)
    (squares,) = call(join_kernel, [jax.ShapeDtypeStruct((8, 1, 128), F32)], [gathered])
    all_squares = exchange(squares, TP)
    entries = 3 * 256 * 2048
    shard = jax.ShapeDtypeStruct((3, 128, 256), F32)
    fixed = [factors, master_weights, mine, mate, line, back, front]
    args = [all_squares, gathered, far_first, far_last] + held_in_hbm(fixed)
    new_weights, steps, weight_copies = call(
        lambda *refs: update_kernel(entries, *refs),
        [shard, shard, jax.ShapeDtypeStruct((3, 2048, 256), BF)],
        args,
        [
            pltpu.VMEM((3, 128, 256), BF),
            pltpu.VMEM((3, 128, 256), F32),
            pltpu.VMEM((3, 128, 256), F32),
            pltpu.VMEM((3, 128, 256), F32),
            pltpu.VMEM((3, 256, 256), BF),
            pltpu.VMEM((3, 16, 128, 256), BF),
            pltpu.VMEM((3, 2048, 256), BF),
            pltpu.VMEM((3, 2048, 256), BF),
            pltpu.SemaphoreType.DMA((2,)),
            pltpu.SemaphoreType.DMA((3, 2)),
            pltpu.SemaphoreType.DMA((12,)),
            pltpu.SemaphoreType.DMA((14,)),
        ],
        mib=20,
        ins=vmem(4) + hbm(7),
        out_specs=hbm(3),
    )
    return (new_weights, weight_copies, steps, new_moments)


def solution(mesh):
    split = Mesh(mesh.devices.reshape(4, 4, 4, 2), (Z, X, Y, C))
    placed = (
        P(FS, None),
        P(FS, None),
        P(FS, TP),
        P(FS, TP),
        P(FS, TP),
        P(None, FS, TP),
        P(None, FS, None),
        P(None, FS, TP),
    )

    return jax.shard_map(
        on_device,
        mesh=split,
        in_specs=placed,
        out_specs=(P(None, FS, TP), P(None, None, TP), P(None, FS, TP), P(None, FS, TP)),
        check_vma=False,
    )
```
